32 devices in a mesh: ep: 8 (over z, x), tp: 4 (over y, core).
Axes of the slice: x: 2, y: 2, z: 4, core: 2. Of those that a mesh axis runs over, the one named last changes fastest.
Arguments:
- mix_input: bfloat16 [4096, 2048], P('ep', 'tp'), may hold values from -6 to 6
- mix_weight: bfloat16 [2048, 4096], P(None, 'tp'), may hold values from -0.125 to 0.125
- expert_input: bfloat16 [1024, 4096], P('ep', 'tp'), may hold values from -4500 to 4500
- expert_index: int32 [1024, 2], P('ep'), may hold values from 0 to 7, as said below
- route_share: float32 [1024, 2], P('ep'), may hold values from 0.1 to 1
- norm_gain: float32 [4096], replicated, may hold values from 0.1 to 1.9
- gate_weight: bfloat16 [8, 4096, 2048], P('ep', None, 'tp'), may hold values from -0.09375 to 0.09375
- up_weight: bfloat16 [8, 4096, 2048], P('ep', None, 'tp'), may hold values from -0.09375 to 0.09375
- down_weight: bfloat16 [8, 2048, 4096], P('ep', None, 'tp'), may hold values from -0.125 to 0.125
Outputs:
- mixed_rows: bfloat16 [4096, 4096], P('ep', 'tp')
- expert_rows: bfloat16 [1024, 4096], P('ep', 'tp')
The draws below stay inside these ranges and needn't reach their ends.
Inputs may be any that keep to these rules, and one draw needn't show every extreme that they name: `expert_index`: each row names 2 different experts. Within each aligned block of 128 rows (the rows of one index of ep) no expert is named by more than 64 rows, and one expert, the same in every block, is named by exactly 64 rows.
All inputs are finite; a program needn't handle non-finite values.
Results may differ from the reference program's by a relative error of at most 0.007.
Values may be sent and summed in bfloat16 or wider, within the bound.
A program may use at most 64 MiB of HBM per device.

```python
import math
from functools import partial
import jax
import jax.numpy as jnp
from jax import lax

D = 4096
POOL = 2048
FF = 2048
TOP = 2
TOK_EXP = 128
EXPERTS = 8
CAP = 64
TOKENS_MIX = 4096
TOKENS_EXP = 1024
N_EP = 8


def draw_expert_input(key, part):
    key_cols, key_rows, key_noise = jax.random.split(key, 3)
    column = jnp.arange(D, dtype=jnp.float32) / (D - 1)
    col_scale = jnp.exp(math.log(3.0) * column + jax.random.uniform(key_cols, (D,), jnp.float32, 0.0, math.log(10.0)))
    noise = jnp.clip(jax.random.normal(key_noise, (TOKENS_EXP, D), jnp.float32), -5.0, 5.0)
    row_scale = jnp.exp(jax.random.uniform(key_rows, (TOKENS_EXP, 1), jnp.float32, 0.0, math.log(10.0)))
    return (noise * col_scale[None, :] * row_scale).astype(jnp.bfloat16)


def draw_expert_index(key, part):
    key_full, key_rest = jax.random.split(key)
    favored = jax.random.randint(key_full, (), 0, EXPERTS)

    def one_block(block_key):
        key_order, key_rows, key_flip = jax.random.split(block_key, 3)
        others = jax.random.permutation(key_order, EXPERTS - 1).astype(jnp.int32)
        others = others + (others >= favored).astype(jnp.int32)
        row_number = jnp.arange(TOK_EXP, dtype=jnp.int32)
        first = jnp.where(row_number < CAP, favored, others[2 * row_number % (EXPERTS - 1)])
        second = jnp.where(row_number < CAP, others[row_number % (EXPERTS - 1)], others[(2 * row_number + 1) % (EXPERTS - 1)])
        flipped = jax.random.randint(key_flip, (TOK_EXP,), 0, 2)
        pairs = jnp.stack([jnp.where(flipped == 1, second, first), jnp.where(flipped == 1, first, second)], axis=1)
        shuffle = jax.random.permutation(key_rows, TOK_EXP)
        return pairs[shuffle]
    blocks = jax.vmap(one_block)(jax.random.split(key_rest, N_EP))
    return blocks.reshape(N_EP * TOK_EXP, 2).astype(jnp.int32)


def levels(own_key, shape, cuts, least, high):
    gain = 1.0
    for dim, shards_of in cuts:
        draws = jax.random.uniform(jax.random.fold_in(jax.random.fold_in(own_key, 6), dim), (shards_of,), jnp.float32, least / len(cuts), high / len(cuts))
        gain = gain * jnp.repeat(jnp.exp(draws), shape[dim] // shards_of).reshape((-1,) + (1,) * (len(shape) - 1 - dim))
    return gain


def normal_values(rng, shape, width, most, pieces=(), held_as=jnp.bfloat16):
    drawn = width * jax.random.normal(rng, shape, jnp.float32)
    if pieces:
        drawn = drawn * levels(rng, shape, pieces, -0.22, 0.18)
    return jnp.clip(drawn, -most, most).astype(held_as)


def setup_inputs(seed: int = 0) -> dict:
    key_of = jax.random.split(jax.random.key(seed), 10)
    mix_input = normal_values(key_of[0], (TOKENS_MIX, POOL), 1.0, 6.0, ((0, 8), (1, 4)))
    mix_weight = normal_values(key_of[1], (POOL, D), POOL ** -0.5, 0.125, ((1, 4),))
    expert_input = draw_expert_input(jax.random.fold_in(key_of[9], 71), 0)
    expert_index = draw_expert_index(jax.random.fold_in(key_of[9], 71), 0)
    route_share = jnp.clip(jnp.exp(math.log(1.0) - 2.3025851 * jax.random.uniform(key_of[4], (TOKENS_EXP, TOP), jnp.float32) ** levels(key_of[4], (TOKENS_EXP, TOP), ((0, 8),), -0.2, 0.2)), 0.1, 1.0)
    norm_gain = jnp.clip(1.0 + 0.18 * jax.random.normal(key_of[5], (D,), jnp.float32), 0.1, 1.9)
    gate_weight = normal_values(key_of[6], (EXPERTS, D, FF), D ** -0.5, 0.09375, ((0, 8), (2, 4)))
    up_weight = normal_values(key_of[7], (EXPERTS, D, FF), D ** -0.5, 0.09375, ((0, 8), (2, 4)))
    down_weight = normal_values(key_of[8], (EXPERTS, FF, D), FF ** -0.5, 0.125, ((0, 8), (2, 4)))
    return {"mix_input": mix_input, "mix_weight": mix_weight, "expert_input": expert_input, "expert_index": expert_index, "route_share": route_share, "norm_gain": norm_gain, "gate_weight": gate_weight, "up_weight": up_weight, "down_weight": down_weight}


window_reach = 15
norm_eps = 1e-06

def pool_minus_self(extended, first_pos, group_size, channel_base):
    length = extended.shape[0] - window_reach
    channels = extended.shape[1]
    channel = channel_base + jnp.arange(channels, dtype=jnp.int32)
    window = jnp.power(2, channel // group_size + 1).astype(jnp.int32)
    running = jnp.zeros((length, channels), jnp.float32)
    for lag_count in range(window_reach + 1):
        shifted = extended[window_reach - lag_count:window_reach - lag_count + length]
        running = running + jnp.where(lag_count < window[None, :], shifted, 0.0)
    position = first_pos + jnp.arange(length, dtype=jnp.int32)
    counts = jnp.minimum(position[:, None] + 1, window[None, :]).astype(jnp.float32)
    return (running / counts - extended[window_reach:]).astype(jnp.bfloat16)

def slot_targets(indices, experts, capacity):
    flattened = indices.reshape(-1)
    one_hot = (flattened[:, None] == jnp.arange(experts, dtype=jnp.int32)[None, :]).astype(jnp.int32)
    earlier = jnp.cumsum(one_hot, axis=0) - one_hot
    return flattened * capacity + lax.optimization_barrier(jnp.sum(earlier * one_hot, axis=1))

def reference(mix_input, mix_weight, expert_input, expert_index, route_share, norm_gain, gate_weight, up_weight, down_weight):
    extended = jnp.pad(mix_input.astype(jnp.float32), ((window_reach, 0), (0, 0)))
    pooled = pool_minus_self(extended, 0, POOL // 4, 0)
    mixed_rows = jnp.dot(pooled, mix_weight, preferred_element_type=jnp.float32).astype(jnp.bfloat16)
    blocks = expert_index.reshape(N_EP, TOK_EXP, TOP)
    targets = jax.vmap(partial(slot_targets, experts=EXPERTS, capacity=CAP))(blocks)
    expert_of = targets // CAP
    slot_of = targets % CAP
    source = jnp.arange(N_EP, dtype=jnp.int32)[:, None]
    placed = (expert_of * (N_EP * CAP) + source * CAP + slot_of).reshape(-1)
    row_ids = (source * TOK_EXP + jnp.repeat(jnp.arange(TOK_EXP, dtype=jnp.int32), TOP)[None, :]).reshape(-1)
    table = jnp.full((EXPERTS * N_EP * CAP,), TOKENS_EXP, jnp.int32).at[placed].set(row_ids)
    padded = jnp.concatenate([expert_input, jnp.zeros((1, D), jnp.bfloat16)], axis=0)

    def run_expert(operands):
        identity, gate_mat, up_mat, down_mat = operands
        rows_in = padded[identity]
        squares = lax.optimization_barrier(jnp.mean(jnp.square(rows_in.astype(jnp.float32)), axis=1, keepdims=True))
        inverse = lax.rsqrt(squares + norm_eps)
        scaled = (rows_in.astype(jnp.float32) * norm_gain).astype(jnp.bfloat16)
        gate_acts = jnp.dot(scaled, gate_mat, preferred_element_type=jnp.float32) * inverse
        up_acts = jnp.dot(scaled, up_mat, preferred_element_type=jnp.float32) * inverse
        hidden = (jax.nn.silu(gate_acts) * up_acts).astype(jnp.bfloat16)
        return jnp.dot(hidden, down_mat, preferred_element_type=jnp.float32).astype(jnp.bfloat16)
    produced = lax.map(run_expert, (table.reshape(EXPERTS, N_EP * CAP), gate_weight, up_weight, down_weight))
    picked = produced.reshape(EXPERTS * N_EP * CAP, D)[placed].astype(jnp.float32).reshape(TOKENS_EXP, TOP, D)
    shares = route_share / lax.optimization_barrier(jnp.sum(route_share, axis=1, keepdims=True))
    expert_rows = lax.optimization_barrier(jnp.sum(picked * shares[:, :, None], axis=1)).astype(jnp.bfloat16)
    return (mixed_rows, expert_rows)
```

```python
import functools

import jax
import jax.numpy as jnp
from jax import lax
from jax.experimental import pallas as pl
from jax.experimental.pallas import tpu as pltpu
from jax.sharding import PartitionSpec as P

TOP = 2
HALO = 16
STAGES = 8
CHUNKS = 4
GROUPS = 4
norm_eps = 1e-06
LIMIT = 48 * 1024 * 1024
MESH = pl.DeviceIdType.MESH
F32 = jnp.float32
BF16 = jnp.bfloat16

PLAN = (
    ("send", 7), ("send", 5), ("barrier",), ("halo",), ("xown",), ("push", 7), ("send", 1),
    ("push", 5), ("send", 2), ("push", 1), ("push", 2), ("pool",), ("pstart", 0), ("xrel",),
    ("push2", 2), ("push2", 1), ("send", 6), ("send", 3), ("send", 4), ("pstart", 3),
    ("ownsel",), ("recv", 7), ("expert", 0, 1), ("push", 6), ("nrecv", 2), ("prelay", 0),
    ("prelay", 3), ("recv", 5), ("push", 3), ("relay", 7), ("expert", 2, 1), ("hrelay", 0, 1),
    ("push", 4), ("expert", 7, 1), ("push2", 3), ("relay", 5), ("recv", 6), ("expert", 5, 1),
    ("hrelay", 7, 1), ("nrecv", 1), ("hrelay", 2, 1), ("down", 7, 1), ("relay", 6), ("recv", 4),
    ("expert", 1, 1), ("hrelay", 5, 1), ("expert", 6, 1), ("nrecv", 3), ("down", 5, 1),
    ("pstart", 1), ("relay", 4), ("down", 2, 1), ("expert", 3, 1), ("hrelay", 6, 1),
    ("expert", 4, 1), ("down", 6, 1), ("hrelay", 4, 1), ("hrelay", 3, 1), ("pstart", 2),
    ("hrelay", 1, 1), ("down", 1, 1), ("down", 3, 1), ("down", 4, 1), ("prelay", 2),
    ("mixed", 3, 1), ("mixed", 0, 1), ("mixed", 2, 1), ("prelay", 1), ("down", 0, 1),
    ("mixed", 1, 1),
)


def dot(a, b):
    return jnp.dot(a, b, preferred_element_type=F32)


def kernel(
    n_ep, n_tp, cap,
    mix_hbm, x_hbm, idx_hbm, share_hbm, gain_hbm, wm_hbm, wg_hbm, wu_hbm, wd_hbm,
    mixed_ref, rows_ref,
    mix_ref, x_ref, idx_ref, share_ref, gain_ref, wm, wg, wu, wd, out, tok, scaled, inv, hid, pool, prod, ret, halo, wcomb, gathered,
    in_sem, w_sem, halo_sem, xy_send, xy_recv, xc_send, xc_recv, a2a_send, a2a_recv, back_send, back_recv,
    ty_send, ty_recv, tc_send, tc_recv,
    hy_send, hy_recv, hc_send, hc_recv,
    py_send, py_recv, pc_send, pc_recv,
):
    e = lax.axis_index("ep")
    t = lax.axis_index("tp")
    n_y = n_tp // 2
    pair = t + 1 - 2 * lax.rem(t, 2)
    tokens = x_ref.shape[0]
    fb = x_ref.shape[1]
    model = fb * n_tp
    length, channels = mix_ref.shape
    hb = wg.shape[1]
    ncols = wd.shape[1]
    gs = n_ep // STAGES
    half = gs * cap
    piece = length // CHUNKS

    def peer(s):
        return e ^ s

    def members(h):
        return range(h * gs, (h + 1) * gs)

    def others(h):
        return [s for s in members(h) if s]

    inputs = [
        pltpu.make_async_copy(src, dst, in_sem.at[i])
        for i, (src, dst) in enumerate(
            (
                (idx_hbm, idx_ref), (x_hbm, x_ref), (mix_hbm, mix_ref),
                (share_hbm, share_ref), (gain_hbm, gain_ref),
            )
        )
    ]
    for copy in inputs:
        copy.start()
    weights = [
        pltpu.make_async_copy(src, dst, w_sem.at[i])
        for i, (src, dst) in enumerate(
            ((wg_hbm.at[0], wg), (wu_hbm.at[0], wu), (wd_hbm.at[0], wd), (wm_hbm, wm))
        )
    ]
    loaded = set()

    def need(i):
        if i not in loaded:
            loaded.add(i)
            weights[i].wait()

    barrier = pltpu.get_barrier_semaphore()
    for s in range(1, n_ep):
        pl.semaphore_signal(
            barrier, inc=1, device_id=(peer(s), t), device_id_type=MESH
        )
    for s in range(1, n_tp):
        pl.semaphore_signal(
            barrier, inc=1, device_id=(e, lax.rem(t + s, n_tp)), device_id_type=MESH
        )
    for copy in weights:
        copy.start()
    inputs[0].wait()

    dest = jnp.concatenate(
        [jnp.full((1, tokens), peer(s), jnp.int32) for s in range(n_ep)], axis=0
    )
    first = idx_ref[0:1, :] == dest
    second = idx_ref[1:2, :] == dest
    named = jnp.where(first | second, 1.0, 0.0)
    before = lax.broadcasted_iota(jnp.int32, (tokens, tokens), 0) < lax.broadcasted_iota(
        jnp.int32, (tokens, tokens), 1
    )
    slot = dot(named.astype(BF16), jnp.where(before, 1.0, 0.0).astype(BF16))
    slot = jnp.where(named > 0.0, slot, -1.0)
    slot_row = lax.broadcasted_iota(jnp.int32, (cap, tokens), 0).astype(F32)

    def chosen(s):
        return slot[s : s + 1, :] == slot_row

    inputs[1].wait()

    def remote(src, dst, send, recv, dev):
        return pltpu.make_async_remote_copy(
            src_ref=src, dst_ref=dst, send_sem=send, recv_sem=recv,
            device_id=dev, device_id_type=MESH,
        )

    sends = []

    def go(*args):
        copy = remote(*args)
        copy.start()
        sends.append(copy)

    def gather_start(view, ys, yr, cs, cr):
        for d in range(1, n_y):
            go(view(t), view(t), ys.at[d], yr.at[d], (e, lax.rem(t + 2 * d, n_tp)))
        go(view(t), view(t), cs.at[0], cr.at[0], (e, pair))

    def gather_relay(view, ys, yr, cs, cr):
        for d in range(1, n_y):
            got = view(lax.rem(t + n_tp - 2 * d, n_tp))
            remote(got, got, ys.at[d], yr.at[d], (e, pair)).wait_recv()
            go(got, got, cs.at[d], cr.at[d], (e, pair))

    def gather_finish(view, ys, yr, cs, cr):
        for d in range(n_y):
            got = view(lax.rem(pair + n_tp - 2 * d, n_tp))
            remote(got, got, cs.at[d], cr.at[d], (e, pair)).wait_recv()

    def tok_args(s):
        return (lambda b: tok.at[b, s], ty_send.at[s], ty_recv.at[s], tc_send.at[s], tc_recv.at[s])

    def hid_args(h, n):
        return (
            lambda b: hid.at[b, pl.ds(h * half, n * half)],
            hy_send.at[h], hy_recv.at[h], hc_send.at[h], hc_recv.at[h],
        )

    def pool_args(c):
        return (
            lambda b: pool.at[b, pl.ds(c * piece, piece)],
            py_send.at[c], py_recv.at[c], pc_send.at[c], pc_recv.at[c],
        )

    def pick(s, x):
        return dot(jnp.where(chosen(s), 1.0, 0.0).astype(BF16), x).astype(BF16)

    def behind(d):
        return lax.rem(t + n_tp - 2 * d, n_tp)

    def near(s):
        return s < n_ep // 2

    def carry(s, d):
        b = behind(d)
        go(out.at[s, d], tok.at[b, s], a2a_send.at[s, d], a2a_recv.at[s, d], (peer(s), t))

    def send(h):
        for s in others(h):
            out[s, 0] = pick(s, x_ref[...])

    def push(h):
        for s in others(h):
            carry(s, 0)

    def xown():
        for d in range(1, n_y):
            go(x_ref, gathered.at[t], xy_send.at[d], xy_recv.at[d], (e, lax.rem(t + 2 * d, n_tp)))
        go(x_ref, gathered.at[t], xc_send.at[0], xc_recv.at[0], (e, pair))

    def xrel():
        gather_relay(lambda b: gathered.at[b], xy_send, xy_recv, xc_send, xc_recv)

    def push2(h):
        for d in range(1, n_y):
            x = gathered[behind(d)]
            for s in others(h):
                out[s, d] = pick(s, x)
                carry(s, d)

    def ownsel():
        gather_finish(lambda b: gathered.at[b], xy_send, xy_recv, xc_send, xc_recv)
        tok[t, 0] = pick(0, x_ref[...])
        for step in range(1, n_tp):
            b = lax.rem(t + step, n_tp)
            tok[b, 0] = pick(0, gathered[b])

    def nrecv(h):
        for s in others(h):
            for d in range(n_y):
                got = tok.at[behind(d), s]
                remote(got, got, a2a_send.at[s, d], a2a_recv.at[s, d], (e, pair)).wait_recv()
                go(got, got, tc_send.at[s, d], tc_recv.at[s, d], (e, pair))

    def halo_step():
        inputs[2].wait()
        go(mix_ref.at[pl.ds(length - HALO, HALO)], halo, halo_sem.at[0], halo_sem.at[1],
           (lax.rem(e + 1, n_ep), t))

    def pool_step():
        inputs[3].wait()
        inputs[4].wait()
        total = share_ref[0:1, :] + share_ref[1:2, :]
        weight = jnp.where(first, share_ref[0:1, :] / total, 0.0) + jnp.where(
            second, share_ref[1:2, :] / total, 0.0
        )
        spread = jnp.concatenate(
            [jnp.where(chosen(s), weight[s : s + 1, :], 0.0) for s in range(n_ep)], axis=0
        ).T
        high = spread.astype(BF16)
        wcomb[0] = high
        wcomb[1] = (spread - high.astype(F32)).astype(BF16)

        remote(halo, halo, halo_sem.at[0], halo_sem.at[1], (e, pair)).wait_recv()
        group = (t * channels) // (channels * n_tp // GROUPS)
        trailing = jnp.where(e == 0, 0.0, halo[...].astype(F32))
        own = mix_ref[...].astype(F32)
        running = jnp.concatenate([trailing, own], axis=0)
        running = running + pltpu.roll(running, 1, 0)
        for level in range(1, GROUPS):
            wider = running + pltpu.roll(running, 2**level, 0)
            running = jnp.where(group >= level, wider, running)
        window = jnp.int32(2)
        for level in range(1, GROUPS):
            window = jnp.where(group >= level, 2 ** (level + 1), window)
        position = e * length + lax.broadcasted_iota(jnp.int32, (length, 1), 0)
        counts = jnp.minimum(position + 1, window).astype(F32)
        pool[t] = (running[HALO:] / counts - own).astype(BF16)

    def recv(h):
        for s in others(h):
            got = tok.at[t, s]
            remote(got, got, a2a_send.at[s, 0], a2a_recv.at[s, 0], (e, pair)).wait_recv()
            gather_start(*tok_args(s))

    def relay(h):
        for s in members(h):
            gather_relay(*tok_args(s))

    def expert(h, n):
        for s in range(max(h * gs, 1), (h + n) * gs):
            gather_finish(*tok_args(s))

        @pl.loop(h * gs, (h + n) * gs)
        def _(s):
            at = pl.ds(pl.multiple_of(s * cap, cap), cap)
            squares = jnp.zeros((cap, 1), F32)
            for b in range(n_tp):
                x = tok[b, s].astype(F32)
                squares = squares + jnp.sum(x * x, axis=1, keepdims=True)
                cols = slice(b * fb, (b + 1) * fb)
                scaled[at, cols] = (x * gain_ref[:, cols]).astype(BF16)
            inv[at, :] = lax.rsqrt(squares / model + norm_eps)

        need(0)
        need(1)
        at = pl.ds(h * half, n * half)
        wide = min(512, hb)

        @pl.loop(0, hb // wide)
        def _(n):
            cols = pl.ds(pl.multiple_of(n * wide, wide), wide)
            lhs = scaled[at, :]
            g = dot(lhs, wg[:, cols]) * inv[at, :]
            u = dot(lhs, wu[:, cols]) * inv[at, :]
            hid[t, at, cols] = (g / (1.0 + jnp.exp(-g)) * u).astype(BF16)

        gather_start(*hid_args(h, n))

    def down(h, n):
        gather_finish(*hid_args(h, n))
        need(2)
        at = pl.ds(h * half, n * half)
        wide = min(512, ncols)

        @pl.loop(0, ncols // wide)
        def _(n):
            cols = pl.ds(pl.multiple_of(n * wide, wide), wide)
            acc = dot(hid[0, at, :], wd[0:hb, cols])
            for b in range(1, n_tp):
                acc = acc + dot(hid[b, at, :], wd[b * hb : (b + 1) * hb, cols])
            prod[at, cols] = acc.astype(BF16)

        for s in range(h * gs, (h + n) * gs):
            rows = pl.ds(s * cap, cap)
            if s == 0:
                ret[rows, :] = prod[rows, :]
            else:
                go(prod.at[rows], ret.at[rows], back_send.at[s], back_recv.at[s], (peer(s), t))

    def mixed_step(c, n):
        for i in range(c, c + n):
            gather_finish(*pool_args(i))
        need(3)
        at = pl.ds(c * piece, n * piece)
        wide = min(512, ncols)

        @pl.loop(0, ncols // wide)
        def _(n):
            cols = pl.ds(pl.multiple_of(n * wide, wide), wide)
            acc = dot(pool[0, at, :], wm[0:channels, cols])
            for b in range(1, n_tp):
                acc = acc + dot(pool[b, at, :], wm[b * channels : (b + 1) * channels, cols])
            mixed_ref[at, cols] = acc.astype(BF16)

    steps = {
        "send": send, "push": push, "xown": xown, "xrel": xrel, "push2": push2, "ownsel": ownsel, "nrecv": nrecv,
        "halo": halo_step, "pool": pool_step,
        "barrier": lambda: pl.semaphore_wait(barrier, n_ep + n_tp - 2),
        "recv": recv, "relay": relay, "expert": expert, "down": down,
        "hrelay": lambda h, n: gather_relay(*hid_args(h, n)),
        "pstart": lambda c: gather_start(*pool_args(c)),
        "prelay": lambda c: gather_relay(*pool_args(c)),
        "mixed": mixed_step,
    }
    for name, *arg in PLAN:
        steps[name](*arg)

    for s in range(1, n_ep):
        got = ret.at[pl.ds(s * cap, cap)]
        remote(got, got, back_send.at[s], back_recv.at[s], (e, pair)).wait_recv()
    wide = min(512, ncols)

    @pl.loop(0, ncols // wide)
    def _(n):
        cols = pl.ds(pl.multiple_of(n * wide, wide), wide)
        back = ret[:, cols]
        rows_ref[:, cols] = (dot(wcomb[0], back) + dot(wcomb[1], back)).astype(BF16)

    for copy in sends:
        copy.wait_send()


def write_out(mixed_ref, rows_ref, mixed_out, rows_out, done):
    copies = [
        pltpu.make_async_copy(mixed_ref, mixed_out, done.at[0]),
        pltpu.make_async_copy(rows_ref, rows_out, done.at[1]),
    ]
    for copy in copies:
        copy.start()
    for copy in copies:
        copy.wait()


def shards(
    n_ep, n_tp,
    mix_input, mix_weight, expert_input, expert_index, route_share, norm_gain,
    gate_weight, up_weight, down_weight,
):
    length, channels = mix_input.shape
    tokens, fb = expert_input.shape
    model = norm_gain.shape[0]
    hb = gate_weight.shape[2]
    ff = down_weight.shape[1]
    ncols = down_weight.shape[2]
    cap = 2 * tokens * TOP // n_ep
    slots = n_ep * cap
    n_y = n_tp // 2
    vmem = pl.BlockSpec(memory_space=pltpu.VMEM)
    hbm = pl.BlockSpec(memory_space=pltpu.HBM)
    sem = pltpu.SemaphoreType.DMA
    mixed, rows = pl.pallas_call(
        functools.partial(kernel, n_ep, n_tp, cap),
        out_shape=(
            pltpu.VMEM((length, ncols), BF16),
            pltpu.VMEM((tokens, ncols), BF16),
        ),
        in_specs=[hbm] * 9,
        out_specs=(vmem, vmem),
        scratch_shapes=[
            pltpu.VMEM(mix_input.shape, BF16),
            pltpu.VMEM(expert_input.shape, BF16),
            pltpu.VMEM((TOP, tokens), jnp.int32),
            pltpu.VMEM((TOP, tokens), F32),
            pltpu.VMEM((1, model), F32),
            pltpu.VMEM(mix_weight.shape, BF16),
            pltpu.VMEM((model, hb), BF16),
            pltpu.VMEM((model, hb), BF16),
            pltpu.VMEM((ff, ncols), BF16),
            pltpu.VMEM((n_ep, n_y, cap, fb), BF16),
            pltpu.VMEM((n_tp, n_ep, cap, fb), BF16),
            pltpu.VMEM((slots, model), BF16),
            pltpu.VMEM((slots, 1), F32),
            pltpu.VMEM((n_tp, slots, hb), BF16),
            pltpu.VMEM((n_tp, length, channels), BF16),
            pltpu.VMEM((slots, ncols), BF16),
            pltpu.VMEM((slots, ncols), BF16),
            pltpu.VMEM((HALO, channels), BF16),
            pltpu.VMEM((2, tokens, slots), BF16),
            pltpu.VMEM((n_tp, tokens, fb), BF16),
            sem((5,)), sem((4,)), sem((2,)), *[sem((n_y,))] * 4,
            sem((n_ep, n_y)), sem((n_ep, n_y)), sem((n_ep,)), sem((n_ep,)),
            sem((n_ep, n_y)), sem((n_ep, n_y)), sem((n_ep, n_y)), sem((n_ep, n_y)),
            *[sem((STAGES, n_y))] * 4,
            *[sem((CHUNKS, n_y))] * 4,
        ],
        compiler_params=pltpu.CompilerParams(
            collective_id=0, has_side_effects=True, vmem_limit_bytes=LIMIT
        ),
    )(
        *[
            pltpu.with_memory_space_constraint(x, pltpu.HBM)
            for x in (
                mix_input, expert_input, expert_index.T, route_share.T, norm_gain[None, :],
                mix_weight, gate_weight, up_weight, down_weight,
            )
        ]
    )
    return pl.pallas_call(
        write_out,
        out_shape=(
            jax.ShapeDtypeStruct(mixed.shape, BF16),
            jax.ShapeDtypeStruct(rows.shape, BF16),
        ),
        in_specs=[vmem] * 2,
        out_specs=(hbm, hbm),
        scratch_shapes=[sem((2,))],
    )(
        pltpu.with_memory_space_constraint(mixed, pltpu.VMEM),
        pltpu.with_memory_space_constraint(rows, pltpu.VMEM),
    )


def solution(mesh):
    placed = (
        P("ep", "tp"),
        P(None, "tp"),
        P("ep", "tp"),
        P("ep", None),
        P("ep", None),
        P(),
        P("ep", None, "tp"),
        P("ep", None, "tp"),
        P("ep", None, "tp"),
    )
    return jax.shard_map(
        functools.partial(shards, mesh.shape["ep"], mesh.shape["tp"]),
        mesh=mesh,
        in_specs=placed,
        out_specs=(P("ep", "tp"), P("ep", "tp")),
        check_vma=False,
    )
```

```python
import functools

import jax
import jax.numpy as jnp
from jax import lax
from jax.experimental import pallas as pl
from jax.experimental.pallas import tpu as pltpu
from jax.sharding import PartitionSpec as P

TOP = 2
HALO = 16
STAGES = 8
CHUNKS = 4
GROUPS = 4
norm_eps = 1e-06
LIMIT = 48 * 1024 * 1024
MESH = pl.DeviceIdType.MESH
F32 = jnp.float32
BF16 = jnp.bfloat16

PLAN = (
    ("send", 7), ("barrier",), ("halo",), ("send", 0), ("push", 0), ("push", 7), ("send", 5),
    ("push", 5), ("send", 2), ("push", 2), ("xown",), ("send", 1), ("pool",), ("pstart", 1),
    ("xrel",), ("push2", 0), ("send", 6), ("send", 3), ("push2", 2), ("send", 4), ("recv", 7),
    ("push", 1), ("push2", 1), ("pstart", 3), ("prelay", 1), ("push", 6), ("relay", 7),
    ("recv", 5), ("nrecv", 2), ("ownsel",), ("nrecv", 0), ("scale", 7, 1), ("push", 3),
    ("gu", 7, 1), ("scale", 2, 1), ("push", 4), ("expert", 7, 1), ("gu", 2, 1), ("expert", 2, 1),
    ("relay", 5), ("recv", 6), ("push2", 3), ("scale", 5, 1), ("hrelay", 7, 1), ("nrecv", 1),
    ("prelay", 3), ("gu", 5, 1), ("expert", 5, 1), ("hrelay", 2, 1), ("down", 7, 1),
    ("scale", 1, 1), ("recv", 4), ("gu", 1, 1), ("relay", 6), ("expert", 1, 1), ("scale", 6, 1),
    ("hrelay", 5, 1), ("gu", 6, 1), ("nrecv", 3), ("expert", 6, 1), ("pstart", 0),
    ("down", 5, 1), ("scale", 3, 1), ("down", 2, 1), ("relay", 4), ("gu", 3, 1),
    ("hrelay", 6, 1), ("expert", 3, 1), ("hrelay", 1, 1), ("scale", 4, 1), ("gu", 4, 1),
    ("expert", 4, 1), ("down", 6, 1), ("scale", 0, 1), ("pstart", 2), ("hrelay", 3, 1),
    ("gu", 0, 1), ("down", 1, 1), ("mixed", 3, 1), ("prelay", 0), ("down", 3, 1),
    ("hrelay", 4, 1), ("down", 4, 1), ("expert", 0, 1), ("comb", 7, 1), ("mixed", 0, 1),
    ("prelay", 2), ("comb", 5, 1), ("hrelay", 0, 1), ("comb", 6, 1), ("mixed", 1, 1),
    ("mixed", 2, 1), ("down", 0, 1), ("comb", 0, 4), ("comb", 4, 1),
)


def dot(a, b):
    return jnp.dot(a, b, preferred_element_type=F32)


def kernel(
    n_ep, n_tp, cap,
    mix_hbm, x_hbm, idx_hbm, share_hbm, gain_hbm, wm_hbm, wg_hbm, wu_hbm, wd_hbm,
    mixed_ref, rows_ref,
    mix_ref, x_ref, idx_ref, share_ref, gain_ref, wm, wg, wu, wd, out, tok, scaled, inv, hid, pool, prod, ret, halo, wcomb, gathered, total,
    in_sem, w_sem, halo_sem, xy_send, xy_recv, xc_send, xc_recv, a2a_send, a2a_recv, back_send, back_recv,
    ty_send, ty_recv, tc_send, tc_recv,
    hy_send, hy_recv, hc_send, hc_recv,
    py_send, py_recv, pc_send, pc_recv,
):
    e = lax.axis_index("ep")
    t = lax.axis_index("tp")
    n_y = n_tp // 2
    pair = t + 1 - 2 * lax.rem(t, 2)
    tokens = x_ref.shape[0]
    fb = x_ref.shape[1]
    model = fb * n_tp
    length, channels = mix_ref.shape
    hb = wg.shape[1]
    ncols = wd.shape[1]
    gs = n_ep // STAGES
    half = gs * cap
    piece = length // CHUNKS

    def peer(s):
        return e ^ s

    def members(h):
        return range(h * gs, (h + 1) * gs)

    def others(h):
        return [s for s in members(h) if s]

    inputs = [
        pltpu.make_async_copy(src, dst, in_sem.at[i])
        for i, (src, dst) in enumerate(
            (
                (idx_hbm, idx_ref), (x_hbm, x_ref), (mix_hbm, mix_ref),
                (share_hbm, share_ref), (gain_hbm, gain_ref),
            )
        )
    ]
    weights = [
        pltpu.make_async_copy(src, dst, w_sem.at[i])
        for i, (src, dst) in enumerate(
            ((wg_hbm.at[0], wg), (wu_hbm.at[0], wu), (wd_hbm.at[0], wd), (wm_hbm, wm))
        )
    ]
    loaded = set()

    def need(i):
        if i not in loaded:
            loaded.add(i)
            weights[i].wait()

    barrier = pltpu.get_barrier_semaphore()
    for s in range(1, n_ep):
        pl.semaphore_signal(
            barrier, inc=1, device_id=(peer(s), t), device_id_type=MESH
        )
    for s in range(1, n_tp):
        pl.semaphore_signal(
            barrier, inc=1, device_id=(e, lax.rem(t + s, n_tp)), device_id_type=MESH
        )
    for copy in inputs + weights:
        copy.start()
    inputs[0].wait()

    dest = jnp.concatenate(
        [jnp.full((1, tokens), peer(s), jnp.int32) for s in range(n_ep)], axis=0
    )
    first = idx_ref[0:1, :] == dest
    second = idx_ref[1:2, :] == dest
    named = jnp.where(first | second, 1.0, 0.0)
    before = lax.broadcasted_iota(jnp.int32, (tokens, tokens), 0) < lax.broadcasted_iota(
        jnp.int32, (tokens, tokens), 1
    )
    slot = dot(named.astype(BF16), jnp.where(before, 1.0, 0.0).astype(BF16))
    slot = jnp.where(named > 0.0, slot, -1.0)
    slot_row = lax.broadcasted_iota(jnp.int32, (cap, tokens), 0).astype(F32)

    def chosen(s):
        return slot[s : s + 1, :] == slot_row

    inputs[1].wait()

    def remote(src, dst, send, recv, dev):
        return pltpu.make_async_remote_copy(
            src_ref=src, dst_ref=dst, send_sem=send, recv_sem=recv,
            device_id=dev, device_id_type=MESH,
        )

    sends = []

    def go(*args):
        copy = remote(*args)
        copy.start()
        sends.append(copy)

    def gather_start(view, ys, yr, cs, cr):
        for d in range(1, n_y):
            go(view(t), view(t), ys.at[d], yr.at[d], (e, lax.rem(t + 2 * d, n_tp)))
        go(view(t), view(t), cs.at[0], cr.at[0], (e, pair))

    def gather_relay(view, ys, yr, cs, cr):
        for d in range(1, n_y):
            got = view(lax.rem(t + n_tp - 2 * d, n_tp))
            remote(got, got, ys.at[d], yr.at[d], (e, pair)).wait_recv()
            go(got, got, cs.at[d], cr.at[d], (e, pair))

    def gather_finish(view, ys, yr, cs, cr):
        for d in range(n_y):
            got = view(lax.rem(pair + n_tp - 2 * d, n_tp))
            remote(got, got, cs.at[d], cr.at[d], (e, pair)).wait_recv()

    def tok_args(s):
        return (lambda b: tok.at[b, s], ty_send.at[s], ty_recv.at[s], tc_send.at[s], tc_recv.at[s])

    def hid_args(h, n):
        return (
            lambda b: hid.at[b, pl.ds(h * half, n * half)],
            hy_send.at[h], hy_recv.at[h], hc_send.at[h], hc_recv.at[h],
        )

    def pool_args(c):
        return (
            lambda b: pool.at[b, pl.ds(c * piece, piece)],
            py_send.at[c], py_recv.at[c], pc_send.at[c], pc_recv.at[c],
        )

    def pick(s, x):
        return dot(jnp.where(chosen(s), 1.0, 0.0).astype(BF16), x).astype(BF16)

    def behind(d):
        return lax.rem(t + n_tp - 2 * d, n_tp)

    def near(s):
        return s < n_ep // 2

    def carry(s, d):
        b = behind(d)
        go(out.at[s, d], tok.at[b, s], a2a_send.at[s, d], a2a_recv.at[s, d], (peer(s), t))

    def send(h):
        for s in others(h):
            out[s, 0] = pick(s, x_ref[...])

    def push(h):
        for s in others(h):
            carry(s, 0)

    def xown():
        for d in range(1, n_y):
            go(x_ref, gathered.at[t], xy_send.at[d], xy_recv.at[d], (e, lax.rem(t + 2 * d, n_tp)))
        go(x_ref, gathered.at[t], xc_send.at[0], xc_recv.at[0], (e, pair))

    def xrel():
        gather_relay(lambda b: gathered.at[b], xy_send, xy_recv, xc_send, xc_recv)

    def push2(h):
        for d in range(1, n_y):
            x = gathered[behind(d)]
            for s in others(h):
                out[s, d] = pick(s, x)
                carry(s, d)

    def ownsel():
        gather_finish(lambda b: gathered.at[b], xy_send, xy_recv, xc_send, xc_recv)
        tok[t, 0] = pick(0, x_ref[...])
        for step in range(1, n_tp):
            b = lax.rem(t + step, n_tp)
            tok[b, 0] = pick(0, gathered[b])

    def nrecv(h):
        for s in others(h):
            for d in range(n_y):
                got = tok.at[behind(d), s]
                remote(got, got, a2a_send.at[s, d], a2a_recv.at[s, d], (e, pair)).wait_recv()
                go(got, got, tc_send.at[s, d], tc_recv.at[s, d], (e, pair))

    def halo_step():
        inputs[2].wait()
        go(mix_ref.at[pl.ds(length - HALO, HALO)], halo, halo_sem.at[0], halo_sem.at[1],
           (lax.rem(e + 1, n_ep), t))

    def pool_step():
        inputs[3].wait()
        inputs[4].wait()
        total = share_ref[0:1, :] + share_ref[1:2, :]
        weight = jnp.where(first, share_ref[0:1, :] / total, 0.0) + jnp.where(
            second, share_ref[1:2, :] / total, 0.0
        )
        for h in range(STAGES):
            spread = jnp.concatenate(
                [jnp.where(chosen(s), weight[s : s + 1, :], 0.0) for s in members(h)], axis=0
            ).T
            high = spread.astype(BF16)
            wcomb[0, h] = high
            wcomb[1, h] = (spread - high.astype(F32)).astype(BF16)

        remote(halo, halo, halo_sem.at[0], halo_sem.at[1], (e, pair)).wait_recv()
        group = (t * channels) // (channels * n_tp // GROUPS)
        trailing = jnp.where(e == 0, 0.0, halo[...].astype(F32))
        own = mix_ref[...].astype(F32)
        running = jnp.concatenate([trailing, own], axis=0)
        running = running + pltpu.roll(running, 1, 0)
        for level in range(1, GROUPS):
            wider = running + pltpu.roll(running, 2**level, 0)
            running = jnp.where(group >= level, wider, running)
        window = jnp.int32(2)
        for level in range(1, GROUPS):
            window = jnp.where(group >= level, 2 ** (level + 1), window)
        position = e * length + lax.broadcasted_iota(jnp.int32, (length, 1), 0)
        counts = jnp.minimum(position + 1, window).astype(F32)
        pool[t] = (running[HALO:] / counts - own).astype(BF16)

    def recv(h):
        for s in others(h):
            got = tok.at[t, s]
            remote(got, got, a2a_send.at[s, 0], a2a_recv.at[s, 0], (e, pair)).wait_recv()
            gather_start(*tok_args(s))

    def relay(h):
        for s in members(h):
            gather_relay(*tok_args(s))

    def scale(h, n):
        for s in range(max(h * gs, 1), (h + n) * gs):
            gather_finish(*tok_args(s))

        @pl.loop(h * gs, (h + n) * gs)
        def _(s):
            at = pl.ds(pl.multiple_of(s * cap, cap), cap)
            squares = jnp.zeros((cap, 1), F32)
            for b in range(n_tp):
                x = tok[b, s].astype(F32)
                squares = squares + jnp.sum(x * x, axis=1, keepdims=True)
                cols = slice(b * fb, (b + 1) * fb)
                scaled[at, cols] = (x * gain_ref[:, cols]).astype(BF16)
            inv[at, :] = lax.rsqrt(squares / model + norm_eps)

    def tall(x):
        return jnp.concatenate([x, x], axis=0) if x.shape[0] <= 64 else x

    def hidden(h, n, cols):
        need(0)
        need(1)
        at = pl.ds(h * half, n * half)
        lhs = tall(scaled[at, :])
        g = dot(lhs, wg[:, cols])[: n * half] * inv[at, :]
        u = dot(lhs, wu[:, cols])[: n * half] * inv[at, :]
        hid[t, at, cols] = (g / (1.0 + jnp.exp(-g)) * u).astype(BF16)

    cut = hb // 2 if hb % 256 == 0 else 0

    def gu(h, n):
        if cut:
            hidden(h, n, slice(0, cut))

    def expert(h, n):
        hidden(h, n, slice(cut, hb))
        gather_start(*hid_args(h, n))

    def down(h, n):
        gather_finish(*hid_args(h, n))
        need(2)
        at = pl.ds(h * half, n * half)
        wide = min(512, ncols)
        lhs = tall(jnp.concatenate([hid[b, at, :] for b in range(n_tp)], axis=1))
        for n0 in range(0, ncols, wide):
            cols = slice(n0, n0 + wide)
            prod[at, cols] = dot(lhs, wd[:, cols])[: n * half].astype(BF16)

        for s in range(h * gs, (h + n) * gs):
            rows = pl.ds(s * cap, cap)
            if s == 0:
                ret[rows, :] = prod[rows, :]
            else:
                go(prod.at[rows], ret.at[rows], back_send.at[s], back_recv.at[s], (peer(s), t))

    combs = [step for step in PLAN if step[0] == "comb"]

    def comb(h, n):
        for s in range(max(h * gs, 1), (h + n) * gs):
            got = ret.at[pl.ds(s * cap, cap)]
            remote(got, got, back_send.at[s], back_recv.at[s], (e, pair)).wait_recv()
        wide = min(512, ncols)
        for n0 in range(0, ncols, wide):
            cols = slice(n0, n0 + wide)
            acc = None if ("comb", h, n) == combs[0] else total[:, cols]
            for i in range(h, h + n):
                back = ret[pl.ds(i * half, half), cols]
                for part in range(2):
                    term = dot(wcomb[part, i], back)
                    acc = term if acc is None else acc + term
            if ("comb", h, n) == combs[-1]:
                rows_ref[:, cols] = acc.astype(BF16)
            else:
                total[:, cols] = acc

    def mixed_step(c, n):
        for i in range(c, c + n):
            gather_finish(*pool_args(i))
        need(3)
        at = pl.ds(c * piece, n * piece)
        wide = min(512, ncols)

        @pl.loop(0, ncols // wide)
        def _(n):
            cols = pl.ds(pl.multiple_of(n * wide, wide), wide)
            acc = dot(pool[0, at, :], wm[0:channels, cols])
            for b in range(1, n_tp):
                acc = acc + dot(pool[b, at, :], wm[b * channels : (b + 1) * channels, cols])
            mixed_ref[at, cols] = acc.astype(BF16)

    steps = {
        "send": send, "push": push, "xown": xown, "xrel": xrel, "push2": push2, "ownsel": ownsel, "nrecv": nrecv,
        "halo": halo_step, "pool": pool_step,
        "barrier": lambda: pl.semaphore_wait(barrier, n_ep + n_tp - 2),
        "recv": recv, "relay": relay, "scale": scale, "gu": gu, "expert": expert, "down": down,
        "comb": comb,
        "hrelay": lambda h, n: gather_relay(*hid_args(h, n)),
        "pstart": lambda c: gather_start(*pool_args(c)),
        "prelay": lambda c: gather_relay(*pool_args(c)),
        "mixed": mixed_step,
    }
    for name, *arg in PLAN:
        steps[name](*arg)

    for copy in sends:
        copy.wait_send()


def write_out(mixed_ref, rows_ref, mixed_out, rows_out, done):
    copies = [
        pltpu.make_async_copy(mixed_ref, mixed_out, done.at[0]),
        pltpu.make_async_copy(rows_ref, rows_out, done.at[1]),
    ]
    for copy in copies:
        copy.start()
    for copy in copies:
        copy.wait()


def shards(
    n_ep, n_tp,
    mix_input, mix_weight, expert_input, expert_index, route_share, norm_gain,
    gate_weight, up_weight, down_weight,
):
    length, channels = mix_input.shape
    tokens, fb = expert_input.shape
    model = norm_gain.shape[0]
    hb = gate_weight.shape[2]
    ff = down_weight.shape[1]
    ncols = down_weight.shape[2]
    cap = 2 * tokens * TOP // n_ep
    slots = n_ep * cap
    n_y = n_tp // 2
    vmem = pl.BlockSpec(memory_space=pltpu.VMEM)
    hbm = pl.BlockSpec(memory_space=pltpu.HBM)
    sem = pltpu.SemaphoreType.DMA
    mixed, rows = pl.pallas_call(
        functools.partial(kernel, n_ep, n_tp, cap),
        out_shape=(
            pltpu.VMEM((length, ncols), BF16),
            pltpu.VMEM((tokens, ncols), BF16),
        ),
        in_specs=[hbm] * 9,
        out_specs=(vmem, vmem),
        scratch_shapes=[
            pltpu.VMEM(mix_input.shape, BF16),
            pltpu.VMEM(expert_input.shape, BF16),
            pltpu.VMEM((TOP, tokens), jnp.int32),
            pltpu.VMEM((TOP, tokens), F32),
            pltpu.VMEM((1, model), F32),
            pltpu.VMEM(mix_weight.shape, BF16),
            pltpu.VMEM((model, hb), BF16),
            pltpu.VMEM((model, hb), BF16),
            pltpu.VMEM((ff, ncols), BF16),
            pltpu.VMEM((n_ep, n_y, cap, fb), BF16),
            pltpu.VMEM((n_tp, n_ep, cap, fb), BF16),
            pltpu.VMEM((slots, model), BF16),
            pltpu.VMEM((slots, 1), F32),
            pltpu.VMEM((n_tp, slots, hb), BF16),
            pltpu.VMEM((n_tp, length, channels), BF16),
            pltpu.VMEM((slots, ncols), BF16),
            pltpu.VMEM((slots, ncols), BF16),
            pltpu.VMEM((HALO, channels), BF16),
            pltpu.VMEM((2, STAGES, tokens, slots // STAGES), BF16),
            pltpu.VMEM((n_tp, tokens, fb), BF16),
            pltpu.VMEM((tokens, ncols), F32),
            sem((5,)), sem((4,)), sem((2,)), *[sem((n_y,))] * 4,
            sem((n_ep, n_y)), sem((n_ep, n_y)), sem((n_ep,)), sem((n_ep,)),
            sem((n_ep, n_y)), sem((n_ep, n_y)), sem((n_ep, n_y)), sem((n_ep, n_y)),
            *[sem((STAGES, n_y))] * 4,
            *[sem((CHUNKS, n_y))] * 4,
        ],
        compiler_params=pltpu.CompilerParams(
            collective_id=0, has_side_effects=True, vmem_limit_bytes=LIMIT
        ),
    )(
        *[
            pltpu.with_memory_space_constraint(x, pltpu.HBM)
            for x in (
                mix_input, expert_input, expert_index.T, route_share.T, norm_gain[None, :],
                mix_weight, gate_weight, up_weight, down_weight,
            )
        ]
    )
    return pl.pallas_call(
        write_out,
        out_shape=(
            jax.ShapeDtypeStruct(mixed.shape, BF16),
            jax.ShapeDtypeStruct(rows.shape, BF16),
        ),
        in_specs=[vmem] * 2,
        out_specs=(hbm, hbm),
        scratch_shapes=[sem((2,))],
    )(
        pltpu.with_memory_space_constraint(mixed, pltpu.VMEM),
        pltpu.with_memory_space_constraint(rows, pltpu.VMEM),
    )


def solution(mesh):
    placed = (
        P("ep", "tp"),
        P(None, "tp"),
        P("ep", "tp"),
        P("ep", None),
        P("ep", None),
        P(),
        P("ep", None, "tp"),
        P("ep", None, "tp"),
        P("ep", None, "tp"),
    )
    return jax.shard_map(
        functools.partial(shards, mesh.shape["ep"], mesh.shape["tp"]),
        mesh=mesh,
        in_specs=placed,
        out_specs=(P("ep", "tp"), P("ep", "tp")),
        check_vma=False,
    )
```
